256 devices in a mesh: sp: 32 (over z, x), tp: 8 (over y, core).
Axes of the slice: x: 4, y: 4, z: 8, core: 2. Of those that a mesh axis runs over, the one named last changes fastest.
Arguments:
- activations: bfloat16 [16384, 1024], P(('sp', 'tp')), may hold values from -8 to 8, as said below
- input_gain: float32 [1024], replicated, may hold values from 0.5 to 1.5
- query_weight: bfloat16 [1024, 1024], P(None, 'tp'), may hold values from -0.1875 to 0.1875
- key_weight: bfloat16 [1024, 1024], P(None, 'tp'), may hold values from -0.375 to 0.375
- value_weight: bfloat16 [1024, 1024], P(None, 'tp'), may hold values from -0.1875 to 0.1875
- stop_offset: float32 [16], P('tp'), may hold values from -16 to 0, as said below
- output_weight: bfloat16 [1024, 1024], P('tp'), may hold values from -0.1875 to 0.1875
- output_gain: float32 [1024], replicated, may hold values from 0.5 to 1.5
Outputs:
- layer_out: bfloat16 [16384, 1024], P(('sp', 'tp'))
The draws below stay inside these ranges and needn't reach their ends.
Inputs may be any that keep to these rules, and one draw needn't show every extreme that they name: activations are noise of about unit size plus a mean vector of about unit size shared by each aligned block of 512 rows and different between runs; each row as a whole may also be scaled by a factor between 0.25 and 2; the result is clipped to the range. `stop_offset`: each entry equals minus the natural logarithm of 16384, minus 2, plus the natural logarithm of 3, plus a number between 0 and 0.7.
All inputs are finite; a program needn't handle non-finite values.
Results may differ from the reference program's by a relative error of at most 0.015.
Values may be sent and summed in bfloat16 or wider, within the bound.
No kernel may reach another device: no remote copies, remote signals or barrier semaphores. Data moves between devices by JAX's collectives and lax.ppermute only.
A program may use at most 128 MiB of HBM per device.

```python
import jax
import jax.numpy as jnp
from jax import lax

D = 1024
HEADS = 16
HEAD_DIM = 64
TOK_DEV = 512
TOKENS = 16384


def draw_activations(key, part):
    noise_key, mean_key, scale_key = jax.random.split(key, 3)
    blocks = TOKENS // TOK_DEV
    noise_part = jax.random.normal(noise_key, (blocks, TOK_DEV, D), jnp.float32)
    block_means = jax.random.normal(mean_key, (blocks, 1, D), jnp.float32)
    combined = noise_part + block_means
    return jnp.clip(combined, -8.0, 8.0).reshape(TOKENS, D).astype(jnp.bfloat16)


def draw_stop_offset(key, part):
    center = -jnp.log(jnp.float32(TOKENS)) - 2.0 + jnp.log(jnp.float32(3.0))
    return center + jax.random.uniform(key, (HEADS,), jnp.float32, 0.0, 0.7)


def steps_of(own_key, dims, cuts, least, top_value):
    loudness, own = 1.0, jax.random.fold_in(own_key, 6)
    for position, parts in cuts:
        draws = jnp.exp(jax.random.uniform(jax.random.fold_in(own, position), (parts,), jnp.float32, least / len(cuts), top_value / len(cuts)))
        loudness = loudness * jnp.repeat(draws, dims[position] // parts).reshape([-1 if axis == position else 1 for axis in range(len(dims))])
    return loudness


def centred(rng, dims, width, most, cuts=(), kind=jnp.bfloat16):
    level = steps_of(rng, dims, cuts, -0.22, 0.18) if cuts else 1.0
    drawn = jax.random.normal(rng, dims, jnp.float32) * width * level
    return jnp.minimum(jnp.maximum(drawn, -most), most).astype(kind)


def setup_inputs(seed: int = 0) -> dict:
    arg_keys = jax.random.split(jax.random.key(seed), 9)
    return {
        "activations": draw_activations(jax.random.fold_in(arg_keys[8], 71), 0),
        "input_gain": jnp.clip(1.0 + 0.1 * jax.random.normal(arg_keys[1], (D,), jnp.float32), 0.5, 1.5),
        "query_weight": centred(arg_keys[2], (D, HEADS * HEAD_DIM), D ** -0.5, 0.1875, ((1, 8),)),
        "key_weight": centred(arg_keys[3], (D, HEADS * HEAD_DIM), (D // 4) ** -0.5, 0.375, ((1, 8),)),
        "value_weight": centred(arg_keys[4], (D, HEADS * HEAD_DIM), D ** -0.5, 0.1875, ((1, 8),)),
        "stop_offset": draw_stop_offset(jax.random.fold_in(arg_keys[8], 71), 0),
        "output_weight": centred(arg_keys[6], (HEADS * HEAD_DIM, D), (HEADS * HEAD_DIM) ** -0.5, 0.1875, ((0, 8),)),
        "output_gain": jnp.clip(1.0 + 0.1 * jax.random.normal(arg_keys[7], (D,), jnp.float32), 0.5, 1.5),
    }


epsilon = 1e-06

def scaled_rows(row_block, row_gain):
    widened = row_block.astype(jnp.float32)
    spread = lax.optimization_barrier(jnp.mean(widened * widened, axis=-1, keepdims=True))
    return (widened * lax.rsqrt(spread + epsilon) * row_gain).astype(jnp.bfloat16)

def reference(activations, input_gain, query_weight, key_weight, value_weight, stop_offset, output_weight, output_gain):
    normed = scaled_rows(activations, input_gain)
    query_rows = jnp.dot(normed, query_weight, preferred_element_type=jnp.float32).astype(jnp.bfloat16)
    key_rows = jnp.dot(normed, key_weight, preferred_element_type=jnp.float32).astype(jnp.bfloat16)
    value_rows = jnp.dot(normed, value_weight, preferred_element_type=jnp.float32).astype(jnp.bfloat16)
    blocks = TOKENS // TOK_DEV
    query_blocks = query_rows.reshape(blocks, TOK_DEV, HEADS, HEAD_DIM)
    key_blocks = key_rows.reshape(blocks, TOK_DEV, HEADS, HEAD_DIM)
    value_blocks = value_rows.reshape(blocks, TOK_DEV, HEADS, HEAD_DIM)
    score_scale = HEAD_DIM ** (-0.5)
    offsets = stop_offset.astype(jnp.float32)

    def attend_block(query_index):
        queries = query_blocks[query_index].astype(jnp.float32)
        first_query = query_index * TOK_DEV

        def per_key(key_index):

            def compute(unused):
                key_here = key_blocks[key_index].astype(jnp.float32)
                value_here = value_blocks[key_index].astype(jnp.float32)
                scores = jnp.einsum('thd,shd->hts', queries, key_here, precision=lax.Precision.HIGHEST)
                scores = scores * score_scale + offsets[:, None, None]
                query_pos = first_query + jnp.arange(TOK_DEV, dtype=jnp.int32)
                key_pos = key_index * TOK_DEV + jnp.arange(TOK_DEV, dtype=jnp.int32)
                earlier = key_pos[None, :] < query_pos[:, None]
                log_keep = jnp.where(earlier[None], jax.nn.log_sigmoid(-scores), 0.0)
                within = lax.cumsum(log_keep, axis=2, reverse=True) - log_keep
                weights = jnp.where(earlier[None], jnp.exp(jax.nn.log_sigmoid(scores) + within), 0.0)
                weights = weights.astype(jnp.bfloat16).astype(jnp.float32)
                shard_part = jnp.einsum('hts,shd->thd', weights, value_here, precision=lax.Precision.HIGHEST)
                return (shard_part, lax.optimization_barrier(jnp.sum(log_keep, axis=2)))

            def skipped(unused):
                return (jnp.zeros((TOK_DEV, HEADS, HEAD_DIM), jnp.float32), jnp.zeros((HEADS, TOK_DEV), jnp.float32))
            return lax.cond(key_index <= query_index, compute, skipped, 0)
        block_parts, totals = lax.map(per_key, jnp.arange(blocks, dtype=jnp.int32))
        prefix_sums = jnp.cumsum(totals, axis=0)
        factors = jnp.exp(prefix_sums[-1:] - prefix_sums)
        combined = jnp.einsum('bht,bthd->thd', factors, block_parts, precision=lax.Precision.HIGHEST)
        return combined.astype(jnp.bfloat16)
    attended = lax.map(attend_block, jnp.arange(blocks, dtype=jnp.int32))
    attended = attended.reshape(TOKENS, HEADS * HEAD_DIM)
    projected = jnp.dot(attended, output_weight, preferred_element_type=jnp.float32)
    return scaled_rows(projected, output_gain)
```

```python
import functools

import jax
import jax.numpy as jnp
import numpy as np
from jax import lax
from jax.experimental import pallas as pl
from jax.experimental.pallas import tpu as pltpu
from jax.sharding import PartitionSpec as P


EPS = 1e-06
LOG2E = 1.4426950408889634
CLAMP = 24.0
BLK = 512
GRP = 128
ZS, XS, YS, CS = 8, 4, 4, 2
bf16 = jnp.bfloat16
f32 = jnp.float32
ANY = pl.BlockSpec(memory_space=pl.ANY)
SMEM = pl.BlockSpec(memory_space=pltpu.SMEM)
VMEM = pl.BlockSpec(memory_space=pltpu.VMEM)


def sp_perm(f):
    pairs = []
    for z in range(ZS):
        for x in range(XS):
            d = f(z, x)
            if d is not None:
                pairs.append((z * XS + x, d[0] * XS + d[1]))
    return pairs


def tp_perm(f):
    pairs = []
    for y in range(YS):
        for c in range(CS):
            d = f(y, c)
            pairs.append((y * CS + c, d[0] * CS + d[1]))
    return pairs


def gather_tp(shard):
    same = [shard]
    for k in (1, 2, 3):
        same.append(lax.ppermute(shard, "tp", tp_perm(lambda y, c: ((y + k) % YS, c))))
    other = [lax.ppermute(a, "tp", tp_perm(lambda y, c: (y, 1 - c))) for a in same]
    return same + other


def piece_tp(tp, i):
    y, c = tp // 2, tp % 2
    k = i % 4
    return ((y - k + 4) % 4) * 2 + (c if i < 4 else 1 - c)


def qkv_kernel(tp_ref, *refs):
    pieces = refs[:8]
    gain_ref, wq_ref, wk_ref, wv_ref, q_ref, kv_ref, xs, ks, vs, sems = refs[8:]
    tp = tp_ref[0]
    rows = 64
    copies = []
    for i in range(8):
        at = pl.multiple_of(piece_tp(tp, i) * rows, rows)
        copies.append(pltpu.make_async_copy(pieces[i], xs.at[pl.ds(at, rows)], sems.at[i]))
    for c in copies:
        c.start()
    for c in copies:
        c.wait()
    gain = gain_ref[...]
    for j in range(4):
        part = xs[pl.ds(j * 128, 128)].astype(f32)
        spread = jnp.mean(part * part, axis=-1, keepdims=True)
        normed = (part * lax.rsqrt(spread + EPS) * gain).astype(bf16)
        q = jnp.dot(normed, wq_ref[...], preferred_element_type=f32) * (LOG2E / 8.0)
        q_ref[pl.ds(j * 128, 128)] = q.T.astype(bf16)
        ks[pl.ds(j * 128, 128)] = jnp.dot(normed, wk_ref[...], preferred_element_type=f32)
        vs[pl.ds(j * 128, 128)] = jnp.dot(normed, wv_ref[...], preferred_element_type=f32)
    for m in range(4):
        kv_ref[pl.ds(m * GRP, GRP)] = ks[pl.ds(m, GRP, stride=4)].astype(bf16)
        kv_ref[pl.ds(BLK + m * GRP, GRP)] = vs[pl.ds(m, GRP, stride=4)].T.astype(bf16)


def attn_tile(qs, kvs, off_ref, tri, acc, rem, slot, at, masked):
    keys = kvs[at, pl.ds(0, BLK)]
    vt = jnp.concatenate([kvs[at, pl.ds(BLK + m * GRP, GRP)] for m in range(4)], axis=1)
    zero = jnp.zeros((64, 256), bf16)
    for t in range(2):
        lanes = pl.ds(t * 256, 256)
        qt = jnp.concatenate(
            [qs[slot, pl.ds(t * 256, 128)], qs[slot, pl.ds(t * 256 + 128, 128)]], axis=1
        )
        if masked:
            gap = (
                lax.broadcasted_iota(jnp.int32, (GRP, 256), 1)
                + t * 256
                - 4 * lax.broadcasted_iota(jnp.int32, (GRP, 256), 0)
            )
        for h in range(2):
            qh = jnp.concatenate([qt[:64], zero] if h == 0 else [zero, qt[64:]], axis=0)
            score = jnp.dot(keys, qh, preferred_element_type=f32) + off_ref[h]
            e = jnp.exp2(jnp.minimum(score, CLAMP))
            es = [e[m * GRP : (m + 1) * GRP] for m in range(4)]
            if masked:
                es = [jnp.where(gap > m, es[m], 0.0) for m in range(4)]
            p0 = 1.0 + es[0]
            p1 = p0 * (1.0 + es[1])
            p2 = p1 * (1.0 + es[2])
            p3 = p2 * (1.0 + es[3])
            lg = lax.log2(p3)
            hi = lg.astype(bf16)
            lo = (lg - hi.astype(f32)).astype(bf16)
            suffix = jnp.dot(tri[...], jnp.concatenate([hi, lo], axis=0), preferred_element_type=f32)
            r = rem[slot, pl.ds(h, 1), lanes]
            f = jnp.exp2(suffix + r)
            w = jnp.concatenate(
                [
                    (es[0] * f).astype(bf16),
                    (es[1] * (p0 * f)).astype(bf16),
                    (es[2] * (p1 * f)).astype(bf16),
                    (es[3] * (p2 * f)).astype(bf16),
                ],
                axis=0,
            )
            hs = pl.ds(h * 64, 64)
            acc[slot, hs, lanes] += jnp.dot(
                vt[h * 64 : (h + 1) * 64], w, preferred_element_type=f32
            )
            rem[slot, pl.ds(h, 1), lanes] = r + suffix[0:1]


def attn_kernel(second, sc_ref, off_ref, *refs):
    qin, kvin, tri = refs[:4], refs[4:8], refs[8]
    if second:
        acc1, rem1 = refs[9:11]
        own_ref, o1, o2, o3, r0, r1, r2, r3 = refs[11:19]
        qs, kvs, sems, acc, rem = refs[19:]
    else:
        acc, rem = refs[9:11]
        qs, kvs, sems = refs[11:]
    zq, z0, x, kz0 = sc_ref[0], sc_ref[1], sc_ref[2], sc_ref[3]
    low = z0 * 4 + x
    copies = []
    for i in range(4):
        copies.append(pltpu.make_async_copy(qin[i], qs.at[i], sems.at[i]))
        copies.append(pltpu.make_async_copy(kvin[i], kvs.at[(x + i) % 4], sems.at[4 + i]))
    for c in copies:
        c.start()
    acc[...] = jnp.zeros_like(acc)
    rem[...] = jnp.zeros_like(rem)
    if second:
        @pl.when(z0 == 1)
        def _():
            acc[...] = acc1[...]
            rem[...] = rem1[...]

    for c in copies:
        c.wait()

    def step(i, carry):
        slot = i // 4
        at = 3 - i % 4
        block = kz0 * 4 + at
        live = zq + slot < 4
        own = slot == 0

        @pl.when(live & (jnp.logical_not(own) | (block < low)))
        def _():
            attn_tile(qs, kvs, off_ref, tri, acc, rem, slot, at, False)

        @pl.when(own & (block == low))
        def _():
            attn_tile(qs, kvs, off_ref, tri, acc, rem, slot, at, True)

        return carry

    lax.fori_loop(0, 16, step, 0)
    if second:
        @pl.when(z0 == 0)
        def _():
            for s in range(4):
                for h in range(2):
                    hs = pl.ds(h * 64, 64)
                    acc[s, hs] += jnp.exp2(rem[s, pl.ds(h, 1)]) * acc1[s, hs]
            rem[...] += rem1[...]

        own_ref[...] = acc[0]
        for o, s in ((o1, 1), (o2, 2), (o3, 3)):
            o[...] = acc[s].astype(bf16)
        for r, s in ((r0, 0), (r1, 1), (r2, 2), (r3, 3)):
            r[...] = rem[s]


def combine_kernel(own, a1, a2, a3, r0, r1, r2, out):
    for h in range(2):
        hs = pl.ds(h * 64, 64)
        hr = pl.ds(h, 1)
        beyond = r0[hr]
        total = own[hs] + jnp.exp2(beyond) * a1[hs].astype(f32)
        beyond = beyond + r1[hr]
        total = total + jnp.exp2(beyond) * a2[hs].astype(f32)
        beyond = beyond + r2[hr]
        total = total + jnp.exp2(beyond) * a3[hs].astype(f32)
        out[hs] = total


def combine_rows_kernel(own, a1, a2, a3, r0, r1, r2, out, tmp):
    combine_kernel(own, a1, a2, a3, r0, r1, r2, tmp)
    for j in range(4):
        out[pl.ds(j * 128, 128)] = tmp[:, pl.ds(j * 128, 128)].T.astype(bf16)


def out_kernel(tp_ref, att, gain, *refs):
    ws, out = refs[:8], refs[8]
    tp = tp_ref[0]
    total = jnp.zeros((64, 1024), f32)
    for i in range(8):
        at = pl.multiple_of(piece_tp(tp, i) * 64, 64)
        total += jnp.dot(att[pl.ds(at, 64)], ws[i][...], preferred_element_type=f32)
    spread = jnp.mean(total * total, axis=-1, keepdims=True)
    out[...] = (total * lax.rsqrt(spread + EPS) * gain[...]).astype(bf16)


def cost(flops, nbytes, trans=0):
    return pl.CostEstimate(flops=flops, bytes_accessed=nbytes, transcendentals=trans)


def local(
    activations,
    input_gain,
    query_weight,
    key_weight,
    value_weight,
    stop_offset,
    output_weight,
    output_gain,
):
    tp = lax.axis_index("tp").astype(jnp.int32)
    sp = lax.axis_index("sp").astype(jnp.int32)
    z, x = sp // XS, sp % XS
    zq, z0 = z // 2, z % 2
    tp1 = tp.reshape(1)
    pieces = gather_tp(activations)
    params = pltpu.CompilerParams(vmem_limit_bytes=56 * 1024 * 1024)
    q, kv = pl.pallas_call(
        qkv_kernel,
        out_shape=(
            jax.ShapeDtypeStruct((BLK, 128), bf16),
            jax.ShapeDtypeStruct((2 * BLK, 128), bf16),
        ),
        in_specs=[SMEM] + [ANY] * 8 + [VMEM] * 4,
        out_specs=(VMEM, VMEM),
        scratch_shapes=[
            pltpu.VMEM((BLK, 1024), bf16),
            pltpu.VMEM((BLK, 128), f32),
            pltpu.VMEM((BLK, 128), f32),
            pltpu.SemaphoreType.DMA((8,)),
        ],
        compiler_params=params,
        cost_estimate=cost(2 * BLK * 1024 * 384, 3 << 20),
        name="qkv",
    )(tp1, *pieces, input_gain.reshape(1, -1), query_weight, key_weight, value_weight)

    kv_swap = lax.ppermute(kv, "sp", sp_perm(lambda a, b: (a ^ 1, b)))
    kv_own = [kv] + [
        lax.ppermute(kv, "sp", sp_perm(lambda a, b: (a, (b - k) % XS))) for k in (1, 2, 3)
    ]
    qs = [q] + [
        lax.ppermute(
            q, "sp", sp_perm(lambda a, b: (a - 2 * k, b) if a - 2 * k >= 0 else None)
        )
        for k in (1, 2, 3)
    ]
    kv_other = [kv_swap] + [
        lax.ppermute(kv_swap, "sp", sp_perm(lambda a, b: (a, (b - k) % XS))) for k in (1, 2, 3)
    ]
    w_pieces = gather_tp(output_weight)

    tri = np.triu(np.full((GRP, GRP), -1.0, np.float32))
    tri = jnp.asarray(np.concatenate([tri, tri], axis=1), bf16)
    offsets = stop_offset.astype(f32) * LOG2E
    state = (
        jax.ShapeDtypeStruct((4, 128, BLK), f32),
        jax.ShapeDtypeStruct((4, 8, BLK), f32),
    )
    scratch = [
        pltpu.VMEM((4, BLK, 128), bf16),
        pltpu.VMEM((4, 2 * BLK, 128), bf16),
        pltpu.SemaphoreType.DMA((8,)),
    ]
    est = cost(16 * 2 * 2 * BLK * BLK * 256, 3 << 20, 16 * 2 * 2 * BLK * BLK)
    acc1, rem1 = pl.pallas_call(
        functools.partial(attn_kernel, False),
        out_shape=state,
        in_specs=[SMEM, SMEM] + [ANY] * 8 + [VMEM],
        out_specs=(VMEM, VMEM),
        scratch_shapes=scratch,
        compiler_params=params,
        cost_estimate=est,
        name="attn_a",
    )(jnp.stack([zq, z0, x, z0]), offsets, *qs, *kv_own, tri)
    rem_t = jax.ShapeDtypeStruct((8, BLK), f32)
    part_t = jax.ShapeDtypeStruct((128, BLK), bf16)
    own, o1, o2, o3, r0, r1, r2, r3 = pl.pallas_call(
        functools.partial(attn_kernel, True),
        out_shape=(jax.ShapeDtypeStruct((128, BLK), f32), part_t, part_t, part_t) + (rem_t,) * 4,
        in_specs=[SMEM, SMEM] + [ANY] * 8 + [VMEM] * 3,
        out_specs=(VMEM,) * 8,
        scratch_shapes=scratch + [pltpu.VMEM(s.shape, s.dtype) for s in state],
        compiler_params=params,
        cost_estimate=est,
        name="attn_b",
    )(jnp.stack([zq, z0, x, 1 - z0]), offsets, *qs, *kv_other, tri, acc1, rem1)

    def up(a, k):
        return lax.ppermute(
            a, "sp", sp_perm(lambda i, j: (i + 2 * k, j) if i + 2 * k < ZS else None)
        )

    g1, g2, g3 = up(o1, 1), up(o2, 2), up(o3, 3)
    s1, s2 = up(r1, 1), up(r2, 2)
    attended = pl.pallas_call(
        combine_rows_kernel,
        out_shape=jax.ShapeDtypeStruct((BLK, 128), bf16),
        in_specs=[VMEM] * 7,
        out_specs=VMEM,
        scratch_shapes=[pltpu.VMEM((128, BLK), f32)],
        name="combine",
    )(own, g1, g2, g3, r0, s1, s2)
    mine = lax.all_to_all(attended, "tp", 0, 0, tiled=True)
    return pl.pallas_call(
        out_kernel,
        out_shape=jax.ShapeDtypeStruct((64, 1024), bf16),
        in_specs=[SMEM] + [VMEM] * 10,
        out_specs=VMEM,
        compiler_params=params,
        name="project",
    )(tp1, mine, output_gain.reshape(1, -1), *w_pieces)


def solution(mesh):
    in_specs = (
        P(("sp", "tp"), None),
        P(),
        P(None, "tp"),
        P(None, "tp"),
        P(None, "tp"),
        P("tp"),
        P("tp", None),
        P(),
    )
    out_specs = P(("sp", "tp"), None)
    return jax.shard_map(local, mesh=mesh, in_specs=in_specs, out_specs=out_specs, check_vma=False)
```

```python
import functools

import jax
import jax.numpy as jnp
import numpy as np
from jax import lax
from jax.experimental import pallas as pl
from jax.experimental.pallas import tpu as pltpu
from jax.sharding import PartitionSpec as P


EPS = 1e-06
LOG2E = 1.4426950408889634
CLAMP = 24.0
BLK = 512
GRP = 128
ZS, XS, YS, CS = 8, 4, 4, 2
bf16 = jnp.bfloat16
f32 = jnp.float32
ANY = pl.BlockSpec(memory_space=pl.ANY)
SMEM = pl.BlockSpec(memory_space=pltpu.SMEM)
VMEM = pl.BlockSpec(memory_space=pltpu.VMEM)


def sp_perm(f):
    pairs = []
    for z in range(ZS):
        for x in range(XS):
            d = f(z, x)
            if d is not None:
                pairs.append((z * XS + x, d[0] * XS + d[1]))
    return pairs


def tp_perm(f):
    pairs = []
    for y in range(YS):
        for c in range(CS):
            d = f(y, c)
            pairs.append((y * CS + c, d[0] * CS + d[1]))
    return pairs


def gather_tp(shard):
    same = [shard]
    for k in (1, 2, 3):
        same.append(lax.ppermute(shard, "tp", tp_perm(lambda y, c: ((y + k) % YS, c))))
    other = [lax.ppermute(a, "tp", tp_perm(lambda y, c: (y, 1 - c))) for a in same]
    return same + other


def piece_tp(tp, i):
    y, c = tp // 2, tp % 2
    k = i % 4
    return ((y - k + 4) % 4) * 2 + (c if i < 4 else 1 - c)


def qkv_kernel(tp_ref, *refs):
    pieces = refs[:8]
    gain_ref, wq_ref, wk_ref, wv_ref, q_ref, kv_ref, xs, ks, vs, sems = refs[8:]
    tp = tp_ref[0]
    rows = 64
    copies = []
    for i in range(8):
        at = pl.multiple_of(piece_tp(tp, i) * rows, rows)
        copies.append(pltpu.make_async_copy(pieces[i], xs.at[pl.ds(at, rows)], sems.at[i]))
    for c in copies:
        c.start()
    for c in copies:
        c.wait()
    gain = gain_ref[...]
    for j in range(4):
        part = xs[pl.ds(j * 128, 128)].astype(f32)
        spread = jnp.mean(part * part, axis=-1, keepdims=True)
        normed = (part * lax.rsqrt(spread + EPS) * gain).astype(bf16)
        q = jnp.dot(normed, wq_ref[...], preferred_element_type=f32) * (LOG2E / 8.0)
        q_ref[pl.ds(j * 128, 128)] = q.T.astype(bf16)
        ks[pl.ds(j * 128, 128)] = jnp.dot(normed, wk_ref[...], preferred_element_type=f32)
        vs[pl.ds(j * 128, 128)] = jnp.dot(normed, wv_ref[...], preferred_element_type=f32)
    for m in range(4):
        kv_ref[pl.ds(m * GRP, GRP)] = ks[pl.ds(m, GRP, stride=4)].astype(bf16)
        kv_ref[pl.ds(BLK + m * GRP, GRP)] = vs[pl.ds(m, GRP, stride=4)].T.astype(bf16)


CHAINS = [(t, h) for t in range(2) for h in range(2)]


def exp_part(z, c, e_ref, l_ref, gap=None):
    e = jnp.exp2(jnp.minimum(z, CLAMP))
    es = [e[m * GRP : (m + 1) * GRP] for m in range(4)]
    if gap is not None:
        es = [jnp.where(gap > m, es[m], 0.0) for m in range(4)]
    p = 1.0
    for m in range(4):
        e_ref[c, pl.ds(m * GRP, GRP)] = es[m]
        p = p * (1.0 + es[m])
    lg = lax.log2(p)
    hi = lg.astype(bf16)
    l_ref[c, pl.ds(0, GRP)] = hi
    l_ref[c, pl.ds(GRP, GRP)] = (lg - hi.astype(f32)).astype(bf16)


def weight_part(suffix, r, c, e_ref, w_ref):
    f = jnp.exp2(suffix + r)
    for m in range(4):
        e = e_ref[c, pl.ds(m * GRP, GRP)]
        w_ref[c, pl.ds(m * GRP, GRP)] = (e * f).astype(bf16)
        if m < 3:
            f = f * (1.0 + e)


def masked_tile(ka, vt, qa, tri, acc, rem, bufs, at):
    e_ref, l_ref, w_ref = bufs[0], bufs[2], bufs[4]
    for c, (t, h) in enumerate(CHAINS):
        gap = (
            lax.broadcasted_iota(jnp.int32, (GRP, 256), 1)
            + t * 256
            - 4 * lax.broadcasted_iota(jnp.int32, (GRP, 256), 0)
        )
        z = jnp.dot(ka[at * 2 + h], qa[h, :, pl.ds(t * 256, 256)], preferred_element_type=f32)
        exp_part(z, c, e_ref, l_ref, gap)
    for c, (t, h) in enumerate(CHAINS):
        lanes = pl.ds(t * 256, 256)
        suffix = jnp.dot(tri[...], l_ref[c], preferred_element_type=f32)
        r = rem[0, pl.ds(h, 1), lanes]
        rem[0, pl.ds(h, 1), lanes] = r + suffix[0:1]
        weight_part(suffix, r, c, e_ref, w_ref)
    for c, (t, h) in enumerate(CHAINS):
        hs = pl.ds(h * 64, 64)
        acc[0, hs, pl.ds(t * 256, 256)] += jnp.dot(vt[at, hs], w_ref[c], preferred_element_type=f32)


def tile_loop(n, tile_of, ka, vt, qa, tri, acc, rem, bufs):
    es, ls, ws = bufs[0:2], bufs[2:4], bufs[4:6]

    def sub(i, par):
        sa, ka_at = tile_of(jnp.minimum(i, n - 1))
        sb, _ = tile_of(jnp.clip(i - 1, 0, n - 1))
        sb = jnp.where((i >= 1) & (i - 1 < n), sb, 4)
        sc, vc_at = tile_of(jnp.clip(i - 2, 0, n - 1))
        sc = jnp.where((i >= 2) & (i - 2 < n), sc, 4)
        for c, (t, h) in enumerate(CHAINS):
            lanes = pl.ds(t * 256, 256)
            hs = pl.ds(h * 64, 64)
            z = jnp.dot(ka[ka_at * 2 + h], qa[sa * 2 + h, :, lanes], preferred_element_type=f32)
            suffix = jnp.dot(tri[...], ls[1 - par][c], preferred_element_type=f32)
            o = jnp.dot(vt[vc_at, hs], ws[par][c], preferred_element_type=f32)
            r = rem[sb, pl.ds(h, 1), lanes]
            rem[sb, pl.ds(h, 1), lanes] = r + suffix[0:1]
            weight_part(suffix, r, c, es[1 - par], ws[1 - par])
            acc[sc, hs, lanes] += o
            exp_part(z, c, es[par], ls[par])

    def body(j, carry):
        sub(2 * j, 0)
        sub(2 * j + 1, 1)
        return carry

    lax.fori_loop(0, jnp.where(n > 0, (n + 3) // 2, 0), body, 0)


def prep(qs, kvs, offs, qa, ka, vt):
    lane = lax.broadcasted_iota(jnp.int32, (BLK, 128), 1)
    for a in range(4):
        k = kvs[a, pl.ds(0, BLK)].astype(f32)
        for h in range(2):
            first = (1 - h) * 64
            one = jnp.where((lane >= first) & (lane < first + 3), 1.0, 0.0)
            ka[a * 2 + h] = jnp.where(lane // 64 == h, k, one).astype(bf16)
        for m in range(4):
            vt[a, :, pl.ds(m * GRP, GRP)] = kvs[a, pl.ds(BLK + m * GRP, GRP)]
    row = lax.broadcasted_iota(jnp.int32, (64, 128), 0)
    for h in range(2):
        bias = jnp.where(row == 2, offs[h, 2], 0.0)
        bias = jnp.where(row == 1, offs[h, 1], bias)
        bias = jnp.where(row == 0, offs[h, 0], bias).astype(bf16)
        for s in range(4):
            for j in range(4):
                at = pl.ds(j * 128, 128)
                qa[s * 2 + h, pl.ds(h * 64, 64), at] = qs[s, pl.ds(j * 128 + h * 64, 64)]
                qa[s * 2 + h, pl.ds((1 - h) * 64, 64), at] = bias


def attn_kernel(second, sc_ref, offs_ref, *refs):
    qin, kvin, tri = refs[:4], refs[4:8], refs[8]
    if second:
        acc1, rem1 = refs[9:11]
        own_ref, o1, o2, o3, r0, r1, r2, r3 = refs[11:19]
        scratch = refs[19:]
    else:
        acc_out, rem_out = refs[9:11]
        scratch = refs[11:]
    qs, kvs, sems, acc, rem, qa, ka, vt = scratch[:8]
    bufs = scratch[8:]
    zq, z0, x, kz0 = sc_ref[0], sc_ref[1], sc_ref[2], sc_ref[3]
    low = z0 * 4 + x
    copies = []
    for i in range(4):
        copies.append(pltpu.make_async_copy(qin[i], qs.at[i], sems.at[i]))
        copies.append(pltpu.make_async_copy(kvin[i], kvs.at[(x + i) % 4], sems.at[4 + i]))
    for c in copies:
        c.start()
    acc[...] = jnp.zeros_like(acc)
    rem[...] = jnp.zeros_like(rem)
    if second:
        @pl.when(z0 == 1)
        def _():
            acc[pl.ds(0, 4)] = acc1[...]
            rem[pl.ds(0, 4)] = rem1[...]

    for c in copies:
        c.wait()
    prep(qs, kvs, offs_ref, qa, ka, vt)
    before = jnp.clip(low - kz0 * 4, 0, 4)
    if not second:
        masked_tile(ka, vt, qa, tri, acc, rem, bufs, x)

    def tile_of(i):
        j = i - before
        own = j < 0
        slot = jnp.where(own, 0, 1 + j // 4)
        at = jnp.where(own, before - 1 - i, 3 - j % 4)
        return slot, at

    tile_loop(before + 4 * (3 - zq), tile_of, ka, vt, qa, tri, acc, rem, bufs)
    if second:
        @pl.when(z0 == 0)
        def _():
            for s in range(4):
                for h in range(2):
                    hs = pl.ds(h * 64, 64)
                    acc[s, hs] += jnp.exp2(rem[s, pl.ds(h, 1)]) * acc1[s, hs]
                rem[s] += rem1[s]

        own_ref[...] = acc[0]
        for o, s in ((o1, 1), (o2, 2), (o3, 3)):
            o[...] = acc[s].astype(bf16)
        for r, s in ((r0, 0), (r1, 1), (r2, 2), (r3, 3)):
            r[...] = rem[s]
    else:
        acc_out[...] = acc[pl.ds(0, 4)]
        rem_out[...] = rem[pl.ds(0, 4)]


def combine_kernel(own, a1, a2, a3, r0, r1, r2, out):
    for h in range(2):
        hs = pl.ds(h * 64, 64)
        hr = pl.ds(h, 1)
        beyond = r0[hr]
        total = own[hs] + jnp.exp2(beyond) * a1[hs].astype(f32)
        beyond = beyond + r1[hr]
        total = total + jnp.exp2(beyond) * a2[hs].astype(f32)
        beyond = beyond + r2[hr]
        total = total + jnp.exp2(beyond) * a3[hs].astype(f32)
        out[hs] = total


def combine_rows_kernel(own, a1, a2, a3, r0, r1, r2, out, tmp):
    combine_kernel(own, a1, a2, a3, r0, r1, r2, tmp)
    for j in range(4):
        out[pl.ds(j * 128, 128)] = tmp[:, pl.ds(j * 128, 128)].T.astype(bf16)


def out_kernel(tp_ref, att, gain, *refs):
    ws, out = refs[:8], refs[8]
    tp = tp_ref[0]
    total = jnp.zeros((64, 1024), f32)
    for i in range(8):
        at = pl.multiple_of(piece_tp(tp, i) * 64, 64)
        total += jnp.dot(att[pl.ds(at, 64)], ws[i][...], preferred_element_type=f32)
    spread = jnp.mean(total * total, axis=-1, keepdims=True)
    out[...] = (total * lax.rsqrt(spread + EPS) * gain[...]).astype(bf16)


def cost(flops, nbytes, trans=0):
    return pl.CostEstimate(flops=flops, bytes_accessed=nbytes, transcendentals=trans)


def local(
    activations,
    input_gain,
    query_weight,
    key_weight,
    value_weight,
    stop_offset,
    output_weight,
    output_gain,
):
    tp = lax.axis_index("tp").astype(jnp.int32)
    sp = lax.axis_index("sp").astype(jnp.int32)
    z, x = sp // XS, sp % XS
    zq, z0 = z // 2, z % 2
    tp1 = tp.reshape(1)
    pieces = gather_tp(activations)
    params = pltpu.CompilerParams(vmem_limit_bytes=56 * 1024 * 1024)
    q, kv = pl.pallas_call(
        qkv_kernel,
        out_shape=(
            jax.ShapeDtypeStruct((BLK, 128), bf16),
            jax.ShapeDtypeStruct((2 * BLK, 128), bf16),
        ),
        in_specs=[SMEM] + [ANY] * 8 + [VMEM] * 4,
        out_specs=(VMEM, VMEM),
        scratch_shapes=[
            pltpu.VMEM((BLK, 1024), bf16),
            pltpu.VMEM((BLK, 128), f32),
            pltpu.VMEM((BLK, 128), f32),
            pltpu.SemaphoreType.DMA((8,)),
        ],
        compiler_params=params,
        cost_estimate=cost(2 * BLK * 1024 * 384, 3 << 20),
        name="qkv",
    )(tp1, *pieces, input_gain.reshape(1, -1), query_weight, key_weight, value_weight)

    kv_swap = lax.ppermute(kv, "sp", sp_perm(lambda a, b: (a ^ 1, b)))
    kv_own = [kv] + [
        lax.ppermute(kv, "sp", sp_perm(lambda a, b: (a, (b - k) % XS))) for k in (1, 2, 3)
    ]
    qs = [q] + [
        lax.ppermute(
            q, "sp", sp_perm(lambda a, b: (a - 2 * k, b) if a - 2 * k >= 0 else None)
        )
        for k in (1, 2, 3)
    ]
    kv_other = [kv_swap] + [
        lax.ppermute(kv_swap, "sp", sp_perm(lambda a, b: (a, (b - k) % XS))) for k in (1, 2, 3)
    ]
    w_pieces = gather_tp(output_weight)

    tri = np.triu(np.full((GRP, GRP), -1.0, np.float32))
    tri = jnp.asarray(np.concatenate([tri, tri], axis=1), bf16)
    offset = stop_offset.astype(f32) * LOG2E
    part0 = lax.reduce_precision(offset, 8, 7)
    part1 = lax.reduce_precision(offset - part0, 8, 7)
    offsets = jnp.stack([part0, part1, offset - part0 - part1], axis=1)
    state = (
        jax.ShapeDtypeStruct((4, 128, BLK), f32),
        jax.ShapeDtypeStruct((4, 8, BLK), f32),
    )
    scratch = [
        pltpu.VMEM((4, BLK, 128), bf16),
        pltpu.VMEM((4, 2 * BLK, 128), bf16),
        pltpu.SemaphoreType.DMA((8,)),
        pltpu.VMEM((5, 128, BLK), f32),
        pltpu.VMEM((5, 8, BLK), f32),
        pltpu.VMEM((8, 128, BLK), bf16),
        pltpu.VMEM((8, BLK, 128), bf16),
        pltpu.VMEM((4, 128, BLK), bf16),
    ]
    scratch += [pltpu.VMEM((4, BLK, 256), f32)] * 2
    scratch += [pltpu.VMEM((4, 2 * GRP, 256), bf16)] * 2
    scratch += [pltpu.VMEM((4, BLK, 256), bf16)] * 2
    est = cost(16 * 2 * 2 * BLK * BLK * 256, 3 << 20, 16 * 2 * 2 * BLK * BLK)
    acc1, rem1 = pl.pallas_call(
        functools.partial(attn_kernel, False),
        out_shape=state,
        in_specs=[SMEM, SMEM] + [ANY] * 8 + [VMEM],
        out_specs=(VMEM, VMEM),
        scratch_shapes=scratch,
        compiler_params=params,
        cost_estimate=est,
        name="attn_a",
    )(jnp.stack([zq, z0, x, z0]), offsets, *qs, *kv_own, tri)
    rem_t = jax.ShapeDtypeStruct((8, BLK), f32)
    part_t = jax.ShapeDtypeStruct((128, BLK), bf16)
    own, o1, o2, o3, r0, r1, r2, r3 = pl.pallas_call(
        functools.partial(attn_kernel, True),
        out_shape=(jax.ShapeDtypeStruct((128, BLK), f32), part_t, part_t, part_t) + (rem_t,) * 4,
        in_specs=[SMEM, SMEM] + [ANY] * 8 + [VMEM] * 3,
        out_specs=(VMEM,) * 8,
        scratch_shapes=scratch,
        compiler_params=params,
        cost_estimate=est,
        name="attn_b",
    )(jnp.stack([zq, z0, x, 1 - z0]), offsets, *qs, *kv_other, tri, acc1, rem1)

    def up(a, k):
        return lax.ppermute(
            a, "sp", sp_perm(lambda i, j: (i + 2 * k, j) if i + 2 * k < ZS else None)
        )

    g1, g2, g3 = up(o1, 1), up(o2, 2), up(o3, 3)
    s1, s2 = up(r1, 1), up(r2, 2)
    attended = pl.pallas_call(
        combine_rows_kernel,
        out_shape=jax.ShapeDtypeStruct((BLK, 128), bf16),
        in_specs=[VMEM] * 7,
        out_specs=VMEM,
        scratch_shapes=[pltpu.VMEM((128, BLK), f32)],
        name="combine",
    )(own, g1, g2, g3, r0, s1, s2)
    mine = lax.all_to_all(attended, "tp", 0, 0, tiled=True)
    return pl.pallas_call(
        out_kernel,
        out_shape=jax.ShapeDtypeStruct((64, 1024), bf16),
        in_specs=[SMEM] + [VMEM] * 10,
        out_specs=VMEM,
        compiler_params=params,
        name="project",
    )(tp1, mine, output_gain.reshape(1, -1), *w_pieces)


def solution(mesh):
    in_specs = (
        P(("sp", "tp"), None),
        P(),
        P(None, "tp"),
        P(None, "tp"),
        P(None, "tp"),
        P("tp"),
        P("tp", None),
        P(),
    )
    out_specs = P(("sp", "tp"), None)
    return jax.shard_map(local, mesh=mesh, in_specs=in_specs, out_specs=out_specs, check_vma=False)
```

```python
import functools

import jax
import jax.numpy as jnp
from jax import lax
from jax.experimental import pallas as pl
from jax.experimental.pallas import tpu as pltpu
from jax.sharding import PartitionSpec as P


EPS = 1e-06
LOG2E = 1.4426950408889634
CLAMP = 24.0
BLK = 512
GRP = 128
CK = 32
ZS, XS, YS, CS = 8, 4, 4, 2
bf16 = jnp.bfloat16
f32 = jnp.float32
ANY = pl.BlockSpec(memory_space=pl.ANY)
SMEM = pl.BlockSpec(memory_space=pltpu.SMEM)
VMEM = pl.BlockSpec(memory_space=pltpu.VMEM)


def sp_perm(f):
    pairs = []
    for z in range(ZS):
        for x in range(XS):
            d = f(z, x)
            if d is not None:
                pairs.append((z * XS + x, d[0] * XS + d[1]))
    return pairs


def tp_perm(f):
    pairs = []
    for y in range(YS):
        for c in range(CS):
            d = f(y, c)
            pairs.append((y * CS + c, d[0] * CS + d[1]))
    return pairs


def send(a, axis, perm):
    return lax.ppermute(a, axis, perm)


def along_y(shard):
    return [shard] + [send(shard, "tp", tp_perm(lambda y, c: ((y + k) % YS, c))) for k in (1, 2, 3)]


def both_cores(same):
    other = [send(a, "tp", tp_perm(lambda y, c: (y, 1 - c))) for a in same]
    return same + other


def piece_tp(tp, i):
    y, c = tp // 2, tp % 2
    k = i % 4
    return ((y - k + 4) % 4) * 2 + (c if i < 4 else 1 - c)


def qkv_kernel(*refs):
    pieces = refs[:8]
    gain_ref, w_ref, q_ref, kv_ref, xs, ks, vs, sems = refs[8:]
    tp = lax.axis_index("tp")
    rows = 64
    copies = []
    for i in range(8):
        at = pl.multiple_of(piece_tp(tp, i) * rows, rows)
        piece = pieces[i].at[pl.ds(0, rows)]
        copies.append(pltpu.make_async_copy(piece, xs.at[pl.ds(at, rows)], sems.at[i]))
    for c in copies:
        c.start()
    for c in copies:
        c.wait()
    gain = gain_ref[0:1]
    for j in range(4):
        part = xs[pl.ds(j * 128, 128)].astype(f32)
        spread = jnp.mean(part * part, axis=-1, keepdims=True)
        normed = (part * lax.rsqrt(spread + EPS) * gain).astype(bf16)
        qk = jnp.dot(normed, w_ref[:, pl.ds(0, 256)], preferred_element_type=f32)
        q_ref[pl.ds(j * 128, 128)] = (qk[:, :128] * (LOG2E / 8.0)).T.astype(bf16)
        ks[pl.ds(j * 128, 128)] = qk[:, 128:]
        vs[pl.ds(j * 128, 128)] = jnp.dot(
            normed, w_ref[:, pl.ds(256, 128)], preferred_element_type=f32
        )
        vcut = []
        for m in range(4):
            rows_of = pl.ds(j * 128 + m, CK, stride=4)
            kv_ref[pl.ds(j * 128 + m * CK, CK)] = ks[rows_of].astype(bf16)
            vcut.append(vs[rows_of])
        kv_ref[pl.ds(BLK + j * 128, 128)] = jnp.concatenate(vcut, axis=0).T.astype(bf16)


CHAINS = [(t, h) for t in range(2) for h in range(2)]


def exp_part(z, c, ch, e_ref, l_ref, gap=None):
    p = 1.0
    for m in range(4):
        at = ch * 4 * CK + m * CK
        e = jnp.exp2(jnp.minimum(z[at : at + CK], CLAMP))
        if gap is not None:
            e = jnp.where(gap > 4 * CK * ch + m, e, 0.0)
        e_ref[c, pl.ds(at, CK)] = e
        p = p * (1.0 + e)
    lg = lax.log2(p)
    hi = lg.astype(bf16)
    l_ref[c, pl.ds(ch * CK, CK)] = hi
    l_ref[c, pl.ds(GRP + ch * CK, CK)] = (lg - hi.astype(f32)).astype(bf16)


def weight_part(suffix, r, c, ch, e_ref, w_ref):
    f = jnp.exp2(suffix[ch * CK : (ch + 1) * CK] + r).astype(bf16)
    for m in range(4):
        at = pl.ds(ch * 4 * CK + m * CK, CK)
        e = e_ref[c, at].astype(bf16)
        w_ref[c, at] = e * f
        if m < 3:
            f = f * (jnp.bfloat16(1.0) + e)


def tile_loop(n, unroll, masked_first, tile_of, ka, vt, qa, tri, acc, rem, bufs):
    es, ls, ws = bufs[0:2], bufs[2:4], bufs[4:6]
    slot0, at0 = tile_of(0)
    for c, (t, h) in enumerate(CHAINS):
        gap = None
        if masked_first:
            gap = (
                lax.broadcasted_iota(jnp.int32, (CK, 256), 1)
                + t * 256
                - 4 * lax.broadcasted_iota(jnp.int32, (CK, 256), 0)
            )
        z = jnp.dot(
            ka[at0 * 2 + h], qa[slot0 * 2 + h, :, pl.ds(t * 256, 256)], preferred_element_type=f32
        )
        for ch in range(4):
            exp_part(z, c, ch, es[1], ls[1], gap)

    def values(slot, at, w_ref):
        for c, (t, h) in enumerate(CHAINS):
            hs = pl.ds(h * 64, 64)
            acc[slot, hs, pl.ds(t * 256, 256)] += jnp.dot(
                vt[at, hs], w_ref[c], preferred_element_type=f32
            )

    def sub(s, par):
        sa, ka_at = tile_of(jnp.minimum(s + 1, n - 1))
        sb, _ = tile_of(s)
        sc, vc_at = tile_of(jnp.maximum(s - 1, 0))
        sc = jnp.where(s >= 1, sc, 4)
        for c, (t, h) in enumerate(CHAINS):
            lanes = pl.ds(t * 256, 256)
            hs = pl.ds(h * 64, 64)
            z = jnp.dot(ka[ka_at * 2 + h], qa[sa * 2 + h, :, lanes], preferred_element_type=f32)
            suffix = jnp.dot(tri[...], ls[1 - par][c], preferred_element_type=f32)
            r = rem[sb, pl.ds(h, 1), lanes]
            rem[sb, pl.ds(h, 1), lanes] = r + suffix[0:1]
            for ch in range(4):
                exp_part(z, c, ch, es[par], ls[par])
                weight_part(suffix, r, c, ch, es[1 - par], ws[1 - par])
            acc[sc, hs, lanes] += jnp.dot(vt[vc_at, hs], ws[par][c], preferred_element_type=f32)

    def body(j, carry):
        for u in range(unroll):
            sub(unroll * j + u, u % 2)
        return carry

    lax.fori_loop(0, n // unroll, body, 0)
    last, last_at = tile_of(n - 1)
    if unroll == 4:
        values(last, last_at, ws[0])
        return

    @pl.when(n % 2 == 1)
    def _():
        sub(n - 1, 0)
        values(last, last_at, ws[1])

    @pl.when(n % 2 == 0)
    def _():
        values(last, last_at, ws[0])


def prep_keys(kv, a, ka, vt):
    lane = lax.broadcasted_iota(jnp.int32, (1, 128), 1)
    k = kv[pl.ds(0, BLK)]
    for h in range(2):
        first = (1 - h) * 64
        mine = jnp.where(lane // 64 == h, 1.0, 0.0).astype(bf16)
        ones = jnp.where((lane >= first) & (lane < first + 3), 1.0, 0.0).astype(bf16)
        ka[a * 2 + h] = k * mine + ones
    for m in range(4):
        vt[a, :, pl.ds(m * GRP, GRP)] = kv[pl.ds(BLK + m * GRP, GRP)]


def prep_queries(qs, offs, qa, tri):
    group = lax.broadcasted_iota(jnp.int32, (GRP, 2 * GRP), 0)
    newer = lax.broadcasted_iota(jnp.int32, (GRP, 2 * GRP), 1) % GRP
    tri[...] = jnp.where(newer >= group, -1.0, 0.0).astype(bf16)
    row = lax.broadcasted_iota(jnp.int32, (64, 128), 0)
    for h in range(2):
        offset = jnp.full((64, 128), offs[h] * LOG2E, f32)
        part0 = offset.astype(bf16).astype(f32)
        part1 = (offset - part0).astype(bf16).astype(f32)
        bias = jnp.where(row == 2, offset - part0 - part1, 0.0)
        bias = jnp.where(row == 1, part1, bias)
        bias = jnp.where(row == 0, part0, bias).astype(bf16)
        for s, q in enumerate(qs):
            for j in range(4):
                at = pl.ds(j * 128, 128)
                qa[s * 2 + h, pl.ds(h * 64, 64), at] = q[pl.ds(j * 128 + h * 64, 64)]
                qa[s * 2 + h, pl.ds((1 - h) * 64, 64), at] = bias


def attn_kernel(stage, offs_ref, *refs):
    merge = stage >= 2
    slots = (2, 2, 2, 1, 1)[stage]
    qin, kvin, refs = refs[:slots], refs[slots : slots + 4], refs[slots + 4 :]
    if merge:
        places = {2: (0, 1), 3: (1,), 4: (0,)}[stage]
        prior = [(refs[0], refs[1], p) for p in places]
        refs = refs[2:]
    count = 1 if stage == 3 else 2
    outs, scratch = refs[:count], refs[count:]
    acc, rem, qa, ka, vt, tri = scratch[:6]
    bufs = scratch[6:]
    sp = lax.axis_index("sp")
    z, x = sp // XS, sp % XS
    zq, z0 = z // 2, z % 2
    live1 = jnp.where(zq <= 2, 4, 0)
    live2 = jnp.where(zq <= 1, 4, 0)
    live3 = jnp.where(zq == 0, 4, 0)
    acc[...] = jnp.zeros_like(acc)
    rem[...] = jnp.zeros_like(rem)

    def prep():
        prep_queries(qin, offs_ref, qa, tri)
        for i in range(4):
            prep_keys(kvin[i], (x + i) % 4, ka, vt)

    if stage == 0:
        def tile_of(i):
            own = i <= x
            return jnp.where(own, 0, 1), jnp.where(own, x - i, 3 - (i - x - 1) % 4)

        prep()
        tile_loop(1 + x + live1, 2, True, tile_of, ka, vt, qa, tri, acc, rem, bufs)
    else:
        n = (None, live2 + live3, live2 + live3, live1, 4 * z0)[stage]
        if merge:
            for s, (acc_in, rem_in, p) in enumerate(prior):
                @pl.when((z0 == 1) | (stage == 4))
                def _():
                    acc[s] = acc_in[p]
                    rem[s] = rem_in[p]

        def tile_of(i):
            return i // 4, 3 - i % 4

        @pl.when(n > 0)
        def _():
            prep()
            tile_loop(n, 4, False, tile_of, ka, vt, qa, tri, acc, rem, bufs)

    if not merge:
        outs[0][...] = acc[pl.ds(0, 2)]
        outs[1][...] = rem[pl.ds(0, 2)]
        return

    if stage == 4:
        outs[0][...] = acc[0]
        outs[1][...] = rem[0]
        return

    @pl.when(z0 == 0)
    def _():
        for s, (acc_in, rem_in, p) in enumerate(prior):
            for h in range(2):
                hs = pl.ds(h * 64, 64)
                acc[s, hs] += jnp.exp2(rem[s, pl.ds(h, 1)]) * acc_in[p, hs]
            rem[s] += rem_in[p]

    for s, o in enumerate(outs):
        o[pl.ds(0, 128)] = acc[s].astype(bf16)
        r = rem[s]
        part0 = r.astype(bf16).astype(f32)
        part1 = (r - part0).astype(bf16).astype(f32)
        rows = part0 + pltpu.roll(part1, 2, 0) + pltpu.roll(r - part0 - part1, 4, 0)
        o[pl.ds(128, 16)] = jnp.concatenate([rows, jnp.zeros_like(rows)], axis=0).astype(bf16)


def combine_kernel(own, r0, a1, a2, a3, out, tmp):
    beyond = r0[...]
    tmp[...] = own[...]
    for a in (a1, a2, a3):
        scale = jnp.exp2(beyond)
        for h in range(2):
            hs = pl.ds(h * 64, 64)
            tmp[hs] += scale[h : h + 1] * a[hs].astype(f32)
        parts = a[pl.ds(128, 16)].astype(f32)[0:8]
        beyond = beyond + (parts + pltpu.roll(parts, 6, 0) + pltpu.roll(parts, 4, 0))
    for j in range(4):
        out[pl.ds(j * 128, 128)] = tmp[:, pl.ds(j * 128, 128)].T.astype(bf16)


def out_kernel(att, gain, *refs):
    ws, out = refs[:8], refs[8]
    tp = lax.axis_index("tp")
    total = jnp.zeros((64, 1024), f32)
    for i in range(8):
        at = pl.multiple_of(piece_tp(tp, i) * 64, 64)
        total += jnp.dot(att[pl.ds(at, 64)], ws[i][...], preferred_element_type=f32)
    spread = jnp.mean(total * total, axis=-1, keepdims=True)
    out[...] = (total * lax.rsqrt(spread + EPS) * gain[...]).astype(bf16)


def vmem(mib):
    return pltpu.CompilerParams(vmem_limit_bytes=mib * 1024 * 1024)


def cost(flops, nbytes, trans=0):
    return pl.CostEstimate(flops=flops, bytes_accessed=nbytes, transcendentals=trans)


def local(
    activations,
    input_gain,
    query_weight,
    key_weight,
    value_weight,
    stop_offset,
    output_weight,
    output_gain,
):
    x_same = along_y(activations)
    w_same = along_y(output_weight)
    weights = jnp.concatenate([query_weight, key_weight, value_weight], axis=1)
    own = jnp.pad(activations, ((0, 16), (0, 0)))
    gain = jnp.broadcast_to(input_gain, (8, 1024))
    pieces = both_cores(x_same)
    q, kv = pl.pallas_call(
        qkv_kernel,
        out_shape=(
            jax.ShapeDtypeStruct((BLK, 128), bf16),
            jax.ShapeDtypeStruct((2 * BLK, 128), bf16),
        ),
        in_specs=[ANY] * 8 + [VMEM] * 2,
        out_specs=(VMEM, VMEM),
        scratch_shapes=[
            pltpu.VMEM((BLK, 1024), bf16),
            pltpu.VMEM((BLK, 128), f32),
            pltpu.VMEM((BLK, 128), f32),
            pltpu.SemaphoreType.DMA((8,)),
        ],
        compiler_params=vmem(10),
        cost_estimate=cost(2 * BLK * 1024 * 384, 3 << 20),
        name="qkv",
    )(own, *pieces[1:], gain, weights)

    def along_x(a):
        return [a] + [send(a, "sp", sp_perm(lambda i, j: (i, (j - k) % XS))) for k in (1, 2, 3)]

    kv_swap = send(kv, "sp", sp_perm(lambda i, j: (i ^ 1, j)))
    kv_own = along_x(kv)
    qs = [q] + [
        send(q, "sp", sp_perm(lambda i, j: (i - 2 * k, j) if i - 2 * k >= 0 else None))
        for k in (1, 2, 3)
    ]
    kv_other = along_x(kv_swap)
    w_pieces = both_cores(w_same)

    scratch = [
        pltpu.VMEM((5, 128, BLK), f32),
        pltpu.VMEM((5, 8, BLK), f32),
        pltpu.VMEM((8, 128, BLK), bf16),
        pltpu.VMEM((8, BLK, 128), bf16),
        pltpu.VMEM((4, 128, BLK), bf16),
        pltpu.VMEM((GRP, 2 * GRP), bf16),
        pltpu.VMEM((4, BLK, 256), f32),
        pltpu.VMEM((4, BLK, 256), f32),
        pltpu.VMEM((4, 2 * GRP, 256), bf16),
        pltpu.VMEM((4, 2 * GRP, 256), bf16),
        pltpu.VMEM((4, BLK, 256), bf16),
        pltpu.VMEM((4, BLK, 256), bf16),
    ]
    state = (
        jax.ShapeDtypeStruct((2, 128, BLK), f32),
        jax.ShapeDtypeStruct((2, 8, BLK), f32),
    )
    part_t = jax.ShapeDtypeStruct((144, BLK), bf16)
    last = (
        jax.ShapeDtypeStruct((128, BLK), f32),
        jax.ShapeDtypeStruct((8, BLK), f32),
    )

    def attend(stage, outs, *ins):
        return pl.pallas_call(
            functools.partial(attn_kernel, stage),
            out_shape=outs,
            in_specs=[SMEM] + [VMEM] * len(ins),
            out_specs=(VMEM,) * len(outs),
            scratch_shapes=scratch,
            compiler_params=vmem(24),
            cost_estimate=cost(8 * 2 * 2 * BLK * BLK * 256, 3 << 20, 8 * 2 * 2 * BLK * BLK),
        )(stop_offset, *ins)

    state01 = attend(0, state, *qs[:2], *kv_own)
    state23 = attend(1, state, *qs[2:], *kv_own)
    o2, o3 = attend(2, (part_t, part_t), *qs[2:], *kv_other, *state23)
    (o1,) = attend(3, (part_t,), qs[1], *kv_other, *state01)
    own, r0 = attend(4, last, q, *kv_other, *state01)

    def up(a, k):
        return send(a, "sp", sp_perm(lambda i, j: (i + 2 * k, j) if i + 2 * k < ZS else None))

    g3, g2, g1 = up(o3, 3), up(o2, 2), up(o1, 1)
    attended = pl.pallas_call(
        combine_kernel,
        out_shape=jax.ShapeDtypeStruct((BLK, 128), bf16),
        in_specs=[VMEM] * 5,
        out_specs=VMEM,
        scratch_shapes=[pltpu.VMEM((128, BLK), f32)],
        compiler_params=vmem(4),
        name="combine",
    )(own, r0, g1, g2, g3)
    mine = lax.all_to_all(attended, "tp", 0, 0, tiled=True)
    return pl.pallas_call(
        out_kernel,
        out_shape=jax.ShapeDtypeStruct((64, 1024), bf16),
        in_specs=[VMEM] * 10,
        out_specs=VMEM,
        compiler_params=vmem(8),
        name="project",
    )(mine, output_gain.reshape(1, -1), *w_pieces)


def solution(mesh):
    in_specs = (
        P(("sp", "tp"), None),
        P(),
        P(None, "tp"),
        P(None, "tp"),
        P(None, "tp"),
        P("tp"),
        P("tp", None),
        P(),
    )
    out_specs = P(("sp", "tp"), None)
    return jax.shard_map(local, mesh=mesh, in_specs=in_specs, out_specs=out_specs, check_vma=False)
```

```python
import functools

import jax
import jax.numpy as jnp
from jax import lax
from jax.experimental import pallas as pl
from jax.experimental.pallas import tpu as pltpu
from jax.sharding import PartitionSpec as P


EPS = 1e-06
LOG2E = 1.4426950408889634
CLAMP = 24.0
BLK = 512
GRP = 128
CK = 32
ZS, XS, YS, CS = 8, 4, 4, 2
bf16 = jnp.bfloat16
f32 = jnp.float32
ANY = pl.BlockSpec(memory_space=pl.ANY)
SMEM = pl.BlockSpec(memory_space=pltpu.SMEM)
VMEM = pl.BlockSpec(memory_space=pltpu.VMEM)


def sp_perm(f):
    pairs = []
    for z in range(ZS):
        for x in range(XS):
            d = f(z, x)
            if d is not None:
                pairs.append((z * XS + x, d[0] * XS + d[1]))
    return pairs


def tp_perm(f):
    pairs = []
    for y in range(YS):
        for c in range(CS):
            d = f(y, c)
            pairs.append((y * CS + c, d[0] * CS + d[1]))
    return pairs


def send(a, axis, perm):
    return lax.ppermute(a, axis, perm)


def along_y(shard):
    return [shard] + [send(shard, "tp", tp_perm(lambda y, c: ((y + k) % YS, c))) for k in (1, 2, 3)]


def both_cores(same):
    other = [send(a, "tp", tp_perm(lambda y, c: (y, 1 - c))) for a in same]
    return same + other


def piece_tp(tp, i):
    y, c = tp // 2, tp % 2
    k = i % 4
    return ((y - k + 4) % 4) * 2 + (c if i < 4 else 1 - c)


def qkv_kernel(*refs):
    pieces = refs[:8]
    gain_ref, w_ref, q_ref, kv_ref, xs, ks, vs, sems = refs[8:]
    tp = lax.axis_index("tp")
    rows = 64
    copies = []
    for i in range(8):
        at = pl.multiple_of(piece_tp(tp, i) * rows, rows)
        piece = pieces[i].at[pl.ds(0, rows)]
        copies.append(pltpu.make_async_copy(piece, xs.at[pl.ds(at, rows)], sems.at[i]))
    for c in copies:
        c.start()
    for c in copies:
        c.wait()
    gain = gain_ref[0:1]
    for j in range(4):
        part = xs[pl.ds(j * 128, 128)].astype(f32)
        spread = jnp.mean(part * part, axis=-1, keepdims=True)
        normed = (part * lax.rsqrt(spread + EPS) * gain).astype(bf16)
        qk = jnp.dot(normed, w_ref[:, pl.ds(0, 256)], preferred_element_type=f32)
        q_ref[pl.ds(j * 128, 128)] = (qk[:, :128] * (LOG2E / 8.0)).T.astype(bf16)
        ks[pl.ds(j * 128, 128)] = qk[:, 128:]
        vs[pl.ds(j * 128, 128)] = jnp.dot(
            normed, w_ref[:, pl.ds(256, 128)], preferred_element_type=f32
        )
        vcut = []
        for m in range(4):
            rows_of = pl.ds(j * 128 + m, CK, stride=4)
            kv_ref[pl.ds(j * 128 + m * CK, CK)] = ks[rows_of].astype(bf16)
            vcut.append(vs[rows_of])
        kv_ref[pl.ds(BLK + j * 128, 128)] = jnp.concatenate(vcut, axis=0).T.astype(bf16)


CHAINS = [(t, h) for t in range(2) for h in range(2)]


def exp_part(z, c, ch, e_ref, l_ref, gap=None):
    p = 1.0
    for m in range(4):
        at = ch * 4 * CK + m * CK
        e = jnp.exp2(jnp.minimum(z[at : at + CK], CLAMP))
        if gap is not None:
            e = jnp.where(gap > 4 * CK * ch + m, e, 0.0)
        e_ref[c, pl.ds(at, CK)] = e
        p = p * (1.0 + e)
    lg = lax.log2(p)
    hi = lg.astype(bf16)
    l_ref[c, pl.ds(ch * CK, CK)] = hi
    l_ref[c, pl.ds(GRP + ch * CK, CK)] = (lg - hi.astype(f32)).astype(bf16)


def weight_part(suffix, r, c, ch, e_ref, w_ref):
    f = jnp.exp2(suffix[ch * CK : (ch + 1) * CK] + r).astype(bf16)
    for m in range(4):
        at = pl.ds(ch * 4 * CK + m * CK, CK)
        e = e_ref[c, at].astype(bf16)
        w_ref[c, at] = e * f
        if m < 3:
            f = f * (jnp.bfloat16(1.0) + e)


def tile_loop(n, unroll, masked_first, tile_of, ka, vt, qa, tri, acc, rem, bufs):
    es, ls, ws = bufs[0:2], bufs[2:4], bufs[4:6]
    slot0, at0 = tile_of(0)
    for c, (t, h) in enumerate(CHAINS):
        gap = None
        if masked_first:
            gap = (
                lax.broadcasted_iota(jnp.int32, (CK, 256), 1)
                + t * 256
                - 4 * lax.broadcasted_iota(jnp.int32, (CK, 256), 0)
            )
        z = jnp.dot(
            ka[at0 * 2 + h], qa[slot0 * 2 + h, :, pl.ds(t * 256, 256)], preferred_element_type=f32
        )
        for ch in range(4):
            exp_part(z, c, ch, es[1], ls[1], gap)

    def values(slot, at, w_ref):
        for c, (t, h) in enumerate(CHAINS):
            hs = pl.ds(h * 64, 64)
            acc[slot, hs, pl.ds(t * 256, 256)] += jnp.dot(
                vt[at, hs], w_ref[c], preferred_element_type=f32
            )

    def sub(s, par):
        sa, ka_at = tile_of(jnp.minimum(s + 1, n - 1))
        sb, _ = tile_of(s)
        sc, vc_at = tile_of(jnp.maximum(s - 1, 0))
        sc = jnp.where(s >= 1, sc, 4)
        for c, (t, h) in enumerate(CHAINS):
            lanes = pl.ds(t * 256, 256)
            hs = pl.ds(h * 64, 64)
            z = jnp.dot(ka[ka_at * 2 + h], qa[sa * 2 + h, :, lanes], preferred_element_type=f32)
            suffix = jnp.dot(tri[...], ls[1 - par][c], preferred_element_type=f32)
            r = rem[sb, pl.ds(h, 1), lanes]
            rem[sb, pl.ds(h, 1), lanes] = r + suffix[0:1]
            for ch in range(4):
                exp_part(z, c, ch, es[par], ls[par])
                weight_part(suffix, r, c, ch, es[1 - par], ws[1 - par])
            acc[sc, hs, lanes] += jnp.dot(vt[vc_at, hs], ws[par][c], preferred_element_type=f32)

    def body(j, carry):
        for u in range(unroll):
            sub(unroll * j + u, u % 2)
        return carry

    lax.fori_loop(0, n // unroll, body, 0)
    last, last_at = tile_of(n - 1)
    if unroll == 4:
        values(last, last_at, ws[0])
        return

    @pl.when(n % 2 == 1)
    def _():
        sub(n - 1, 0)
        values(last, last_at, ws[1])

    @pl.when(n % 2 == 0)
    def _():
        values(last, last_at, ws[0])


def prep_keys(kv, a, ka, vt):
    lane = lax.broadcasted_iota(jnp.int32, (1, 128), 1)
    k = kv[pl.ds(0, BLK)]
    for h in range(2):
        first = (1 - h) * 64
        mine = jnp.where(lane // 64 == h, 1.0, 0.0).astype(bf16)
        ones = jnp.where((lane >= first) & (lane < first + 3), 1.0, 0.0).astype(bf16)
        ka[a * 2 + h] = k * mine + ones
    for m in range(4):
        vt[a, :, pl.ds(m * GRP, GRP)] = kv[pl.ds(BLK + m * GRP, GRP)]


def prep_queries(qs, offs, qa, tri):
    group = lax.broadcasted_iota(jnp.int32, (GRP, 2 * GRP), 0)
    newer = lax.broadcasted_iota(jnp.int32, (GRP, 2 * GRP), 1) % GRP
    tri[...] = jnp.where(newer >= group, -1.0, 0.0).astype(bf16)
    row = lax.broadcasted_iota(jnp.int32, (64, 128), 0)
    for h in range(2):
        offset = jnp.full((64, 128), offs[h] * LOG2E, f32)
        part0 = offset.astype(bf16).astype(f32)
        part1 = (offset - part0).astype(bf16).astype(f32)
        bias = jnp.where(row == 2, offset - part0 - part1, 0.0)
        bias = jnp.where(row == 1, part1, bias)
        bias = jnp.where(row == 0, part0, bias).astype(bf16)
        for s, q in enumerate(qs):
            for j in range(4):
                at = pl.ds(j * 128, 128)
                qa[s * 2 + h, pl.ds(h * 64, 64), at] = q[pl.ds(j * 128 + h * 64, 64)]
                qa[s * 2 + h, pl.ds((1 - h) * 64, 64), at] = bias


def attn_kernel(stage, offs_ref, *refs):
    merge = stage >= 2
    slots = (2, 2, 2, 1, 1)[stage]
    fresh = stage in (0, 2)
    given = 4 if fresh else 2
    qin, kvin, refs = refs[:slots], refs[slots : slots + given], refs[slots + given :]
    if merge:
        places = {2: (0, 1), 3: (1,), 4: (0,)}[stage]
        prior = [(refs[0], refs[1], p) for p in places]
        refs = refs[2:]
    count = 1 if stage == 3 else 2
    outs, scratch = refs[:count], refs[count:]
    if fresh:
        ka, vt = scratch[:2]
        scratch = scratch[2:]
    else:
        ka, vt = kvin
    acc, rem, qa, tri = scratch[:4]
    bufs = scratch[4:]
    sp = lax.axis_index("sp")
    z, x = sp // XS, sp % XS
    zq, z0 = z // 2, z % 2
    live1 = jnp.where(zq <= 2, 4, 0)
    live2 = jnp.where(zq <= 1, 4, 0)
    live3 = jnp.where(zq == 0, 4, 0)
    acc[...] = jnp.zeros_like(acc)
    rem[...] = jnp.zeros_like(rem)

    if fresh:
        for i in range(4):
            prep_keys(kvin[i], (x + i) % 4, ka, vt)

    if stage == 0:
        def tile_of(i):
            own = i <= x
            return jnp.where(own, 0, 1), jnp.where(own, x - i, 3 - (i - x - 1) % 4)

        prep_queries(qin, offs_ref, qa, tri)
        tile_loop(1 + x + live1, 2, True, tile_of, ka, vt, qa, tri, acc, rem, bufs)
    else:
        n = (None, live2 + live3, live2 + live3, live1, 4 * z0)[stage]
        if merge:
            for s, (acc_in, rem_in, p) in enumerate(prior):
                @pl.when((z0 == 1) | (stage == 4))
                def _():
                    acc[s] = acc_in[p]
                    rem[s] = rem_in[p]

        def tile_of(i):
            return i // 4, 3 - i % 4

        @pl.when(n > 0)
        def _():
            prep_queries(qin, offs_ref, qa, tri)
            tile_loop(n, 4, False, tile_of, ka, vt, qa, tri, acc, rem, bufs)

    if not merge:
        outs[0][...] = acc[pl.ds(0, 2)]
        outs[1][...] = rem[pl.ds(0, 2)]
        return

    if stage == 4:
        outs[0][...] = acc[0]
        outs[1][...] = rem[0]
        return

    @pl.when(z0 == 0)
    def _():
        for s, (acc_in, rem_in, p) in enumerate(prior):
            for h in range(2):
                hs = pl.ds(h * 64, 64)
                acc[s, hs] += jnp.exp2(rem[s, pl.ds(h, 1)]) * acc_in[p, hs]
            rem[s] += rem_in[p]

    for s, o in enumerate(outs):
        o[pl.ds(0, 128)] = acc[s].astype(bf16)
        r = rem[s]
        part0 = r.astype(bf16).astype(f32)
        part1 = (r - part0).astype(bf16).astype(f32)
        rows = part0 + pltpu.roll(part1, 2, 0) + pltpu.roll(r - part0 - part1, 4, 0)
        o[pl.ds(128, 16)] = jnp.concatenate([rows, jnp.zeros_like(rows)], axis=0).astype(bf16)


def combine_kernel(own, r0, a1, a2, a3, out, tmp):
    beyond = r0[...]
    tmp[...] = own[...]
    for a in (a1, a2, a3):
        scale = jnp.exp2(beyond)
        for h in range(2):
            hs = pl.ds(h * 64, 64)
            tmp[hs] += scale[h : h + 1] * a[hs].astype(f32)
        parts = a[pl.ds(128, 16)].astype(f32)[0:8]
        beyond = beyond + (parts + pltpu.roll(parts, 6, 0) + pltpu.roll(parts, 4, 0))
    for j in range(4):
        out[pl.ds(j * 128, 128)] = tmp[:, pl.ds(j * 128, 128)].T.astype(bf16)


def out_kernel(att, gain, *refs):
    ws, out = refs[:8], refs[8]
    tp = lax.axis_index("tp")
    total = jnp.zeros((64, 1024), f32)
    for i in range(8):
        at = pl.multiple_of(piece_tp(tp, i) * 64, 64)
        total += jnp.dot(att[pl.ds(at, 64)], ws[i][...], preferred_element_type=f32)
    spread = jnp.mean(total * total, axis=-1, keepdims=True)
    out[...] = (total * lax.rsqrt(spread + EPS) * gain[...]).astype(bf16)


def vmem(mib):
    return pltpu.CompilerParams(vmem_limit_bytes=mib * 1024 * 1024)


def cost(flops, nbytes, trans=0):
    return pl.CostEstimate(flops=flops, bytes_accessed=nbytes, transcendentals=trans)


def local(
    activations,
    input_gain,
    query_weight,
    key_weight,
    value_weight,
    stop_offset,
    output_weight,
    output_gain,
):
    x_same = along_y(activations)
    w_same = along_y(output_weight)
    weights = jnp.concatenate([query_weight, key_weight, value_weight], axis=1)
    own = jnp.pad(activations, ((0, 16), (0, 0)))
    gain = jnp.broadcast_to(input_gain, (8, 1024))
    pieces = both_cores(x_same)
    q, kv = pl.pallas_call(
        qkv_kernel,
        out_shape=(
            jax.ShapeDtypeStruct((BLK, 128), bf16),
            jax.ShapeDtypeStruct((2 * BLK, 128), bf16),
        ),
        in_specs=[ANY] * 8 + [VMEM] * 2,
        out_specs=(VMEM, VMEM),
        scratch_shapes=[
            pltpu.VMEM((BLK, 1024), bf16),
            pltpu.VMEM((BLK, 128), f32),
            pltpu.VMEM((BLK, 128), f32),
            pltpu.SemaphoreType.DMA((8,)),
        ],
        compiler_params=vmem(10),
        cost_estimate=cost(2 * BLK * 1024 * 384, 3 << 20),
        name="qkv",
    )(own, *pieces[1:], gain, weights)

    def along_x(a):
        return [a] + [send(a, "sp", sp_perm(lambda i, j: (i, (j - k) % XS))) for k in (1, 2, 3)]

    kv_swap = send(kv, "sp", sp_perm(lambda i, j: (i ^ 1, j)))
    kv_own = along_x(kv)
    qs = [q] + [
        send(q, "sp", sp_perm(lambda i, j: (i - 2 * k, j) if i - 2 * k >= 0 else None))
        for k in (1, 2, 3)
    ]
    kv_other = along_x(kv_swap)
    w_pieces = both_cores(w_same)

    scratch = [
        pltpu.VMEM((5, 128, BLK), f32),
        pltpu.VMEM((5, 8, BLK), f32),
        pltpu.VMEM((8, 128, BLK), bf16),
        pltpu.VMEM((GRP, 2 * GRP), bf16),
        pltpu.VMEM((4, BLK, 256), f32),
        pltpu.VMEM((4, BLK, 256), f32),
        pltpu.VMEM((4, 2 * GRP, 256), bf16),
        pltpu.VMEM((4, 2 * GRP, 256), bf16),
        pltpu.VMEM((4, BLK, 256), bf16),
        pltpu.VMEM((4, BLK, 256), bf16),
    ]
    formed = (
        jax.ShapeDtypeStruct((8, BLK, 128), bf16),
        jax.ShapeDtypeStruct((4, 128, BLK), bf16),
    )
    state = (
        jax.ShapeDtypeStruct((2, 128, BLK), f32),
        jax.ShapeDtypeStruct((2, 8, BLK), f32),
    )
    part_t = jax.ShapeDtypeStruct((144, BLK), bf16)
    last = (
        jax.ShapeDtypeStruct((128, BLK), f32),
        jax.ShapeDtypeStruct((8, BLK), f32),
    )

    def attend(stage, outs, *ins):
        return pl.pallas_call(
            functools.partial(attn_kernel, stage),
            out_shape=outs,
            in_specs=[SMEM] + [VMEM] * len(ins),
            out_specs=(VMEM,) * len(outs),
            scratch_shapes=scratch,
            compiler_params=vmem(24),
            cost_estimate=cost(8 * 2 * 2 * BLK * BLK * 256, 3 << 20, 8 * 2 * 2 * BLK * BLK),
        )(stop_offset, *ins)

    *state01, ka, vt = attend(0, state + formed, *qs[:2], *kv_own)
    state23 = attend(1, state, *qs[2:], ka, vt)
    o2, o3, ka, vt = attend(2, (part_t, part_t) + formed, *qs[2:], *kv_other, *state23)
    (o1,) = attend(3, (part_t,), qs[1], ka, vt, *state01)
    own, r0 = attend(4, last, q, ka, vt, *state01)

    def up(a, k):
        return send(a, "sp", sp_perm(lambda i, j: (i + 2 * k, j) if i + 2 * k < ZS else None))

    g3, g2, g1 = up(o3, 3), up(o2, 2), up(o1, 1)
    attended = pl.pallas_call(
        combine_kernel,
        out_shape=jax.ShapeDtypeStruct((BLK, 128), bf16),
        in_specs=[VMEM] * 5,
        out_specs=VMEM,
        scratch_shapes=[pltpu.VMEM((128, BLK), f32)],
        compiler_params=vmem(4),
        name="combine",
    )(own, r0, g1, g2, g3)
    mine = lax.all_to_all(attended, "tp", 0, 0, tiled=True)
    return pl.pallas_call(
        out_kernel,
        out_shape=jax.ShapeDtypeStruct((64, 1024), bf16),
        in_specs=[VMEM] * 10,
        out_specs=VMEM,
        compiler_params=vmem(8),
        name="project",
    )(mine, output_gain.reshape(1, -1), *w_pieces)


def solution(mesh):
    in_specs = (
        P(("sp", "tp"), None),
        P(),
        P(None, "tp"),
        P(None, "tp"),
        P(None, "tp"),
        P("tp"),
        P("tp", None),
        P(),
    )
    out_specs = P(("sp", "tp"), None)
    return jax.shard_map(local, mesh=mesh, in_specs=in_specs, out_specs=out_specs, check_vma=False)
```
